1024 devices in a mesh: sp: 16 (over x, core), tp: 64 (over z, y).
Axes of the slice: x: 8, y: 8, z: 8, core: 2. Of those that a mesh axis runs over, the one named last changes fastest.
Arguments:
- latents: bfloat16 [4096, 2048], P(('sp', 'tp')), may hold values from -6 to 6
- context: bfloat16 [1024, 2048], P('sp'), may hold values from -6 to 6
- condition: float32 [2048], P('sp'), may hold values from -12 to 12
- context_condition: float32 [2048], P('sp'), may hold values from -12 to 12
- norm_gain: float32 [2048], replicated, may hold values from 0.1 to 1.9
- shift_weight: bfloat16 [2048, 2048], P('sp', 'tp'), may hold values from -0.09375 to 0.09375
- scale_weight: bfloat16 [2048, 2048], P('sp', 'tp'), may hold values from -0.09375 to 0.09375
- gate_weight: bfloat16 [2048, 2048], P('sp', 'tp'), may hold values from -0.125 to 0.125
- query_weight: bfloat16 [2048, 8192], P(None, 'tp'), may hold values from -0.125 to 0.125
- key_weight: bfloat16 [2048, 8192], P(None, 'tp'), may hold values from -0.125 to 0.125
- value_weight: bfloat16 [2048, 8192], P(None, 'tp'), may hold values from -0.125 to 0.125
- subtract_share: float32 [64], P('tp'), may hold values from 0.3 to 0.8
- head_gain: float32 [128], replicated, may hold values from 0.1 to 1.9
- output_weight: bfloat16 [8192, 2048], P('tp'), may hold values from -0.0625 to 0.0625
Outputs:
- updated: bfloat16 [4096, 2048], P(('sp', 'tp'))
The draws below stay inside these ranges and needn't reach their ends.
All inputs are finite; a program needn't handle non-finite values.
Results may differ from the reference program's by a relative error of at most 0.013.
Values may be sent and summed in bfloat16 or wider, within the bound.
A program may use at most 32 MiB of HBM per device.

```python
import math
import jax
import jax.numpy as jnp
from jax import lax

D = 2048
HEAD = 64
VALUE = 128
HEADS = 64
GRID_W = 64
TOKENS = 4096
CTX = 1024


def ramped_draw(base_key):
    position = jnp.arange(D, dtype=jnp.float32) / (D - 1)
    values = jnp.clip(jax.random.normal(base_key, (D,), jnp.float32), -4.0, 4.0)
    growth = jnp.exp(jnp.log(3.0) * position)
    return values * growth


def draw_condition(key, part):
    return ramped_draw(jax.random.fold_in(key, 11))


def draw_context_condition(key, part):
    return ramped_draw(jax.random.fold_in(key, 29))


def block_levels(key, shape, cuts, least, largest):
    def one(dim, shards_of):
        heights = jax.random.uniform(jax.random.fold_in(jax.random.fold_in(key, 6), dim), (shards_of,), jnp.float32, least / len(cuts), largest / len(cuts))
        return jnp.repeat(jnp.exp(heights), shape[dim] // shards_of).reshape((-1,) + (1,) * (len(shape) - dim - 1))

    level = one(*cuts[0])
    for cut in cuts[1:]:
        level = level * one(*cut)
    return level


def centred(rng, dims, spread, limit, cuts=(), kind=jnp.bfloat16):
    array = spread * jax.random.normal(rng, dims, jnp.float32)
    if cuts:
        array = array * block_levels(rng, dims, cuts, -0.22, 0.18)
    return jnp.clip(array, -limit, limit).astype(kind)


def setup_inputs(seed: int = 0) -> dict:
    streams_of = jax.random.split(jax.random.key(seed), 15)
    latents = centred(streams_of[0], (TOKENS, D), 1.0, 6.0, ((0, 1024),))
    context = centred(streams_of[1], (CTX, D), 1.0, 6.0, ((0, 16),))
    condition = draw_condition(jax.random.fold_in(streams_of[14], 71), 0)
    context_condition = draw_context_condition(jax.random.fold_in(streams_of[14], 71), 0)
    norm_gain = jnp.clip(1.0 + 0.18 * jax.random.normal(streams_of[4], (D,), jnp.float32), 0.1, 1.9)
    shift_weight = centred(streams_of[5], (D, D), (2 * D) ** -0.5, 0.09375, ((0, 16), (1, 64)))
    scale_weight = centred(streams_of[6], (D, D), (2 * D) ** -0.5, 0.09375, ((0, 16), (1, 64)))
    gate_weight = centred(streams_of[7], (D, D), D ** -0.5, 0.125, ((0, 16), (1, 64)))
    query_weight = centred(streams_of[8], (D, HEADS * VALUE), D ** -0.5, 0.125, ((1, 64),))
    key_weight = centred(streams_of[9], (D, HEADS * VALUE), D ** -0.5, 0.125, ((1, 64),))
    value_weight = centred(streams_of[10], (D, HEADS * VALUE), D ** -0.5, 0.125, ((1, 64),))
    subtract_share = jnp.clip(0.3 + 0.5 * jax.random.uniform(streams_of[11], (HEADS,), jnp.float32) ** block_levels(streams_of[11], (HEADS,), ((0, 64),), -0.2, 0.2), 0.3, 0.8)
    head_gain = jnp.clip(1.0 + 0.18 * jax.random.normal(streams_of[12], (VALUE,), jnp.float32), 0.1, 1.9)
    output_weight = centred(streams_of[13], (HEADS * VALUE, D), (HEADS * VALUE) ** -0.5, 0.0625, ((0, 64),))
    return dict(latents=latents, context=context, condition=condition, context_condition=context_condition, norm_gain=norm_gain, shift_weight=shift_weight, scale_weight=scale_weight, gate_weight=gate_weight, query_weight=query_weight, key_weight=key_weight, value_weight=value_weight, subtract_share=subtract_share, head_gain=head_gain, output_weight=output_weight)


norm_eps = 1e-06
head_eps = 1e-05
rope_theta = 10000.0
head_scale = 0.8

def rotary_tables(positions):
    quarter = HEAD // 4
    inverse = rope_theta ** (-2.0 * jnp.arange(quarter, dtype=jnp.float32) / (HEAD // 2))
    row_angle = (positions // GRID_W).astype(jnp.float32)[:, None] * inverse[None, :]
    column_angle = (positions % GRID_W).astype(jnp.float32)[:, None] * inverse[None, :]
    angles = jnp.concatenate([row_angle, row_angle, column_angle, column_angle], axis=-1)
    return (jnp.cos(angles), jnp.sin(angles))

def rotate(vectors, cosine, sine_table):
    quarter = HEAD // 4
    pieces = vectors.reshape(vectors.shape[:-1] + (2, 2, quarter))
    turned = jnp.concatenate([-pieces[..., 1:, :], pieces[..., :1, :]], axis=-2).reshape(vectors.shape)
    return vectors * cosine[:, None, :] + turned * sine_table[:, None, :]

def modulate(token_rows, gain_row, shift_row, scale_row):
    widened = token_rows.astype(jnp.float32)
    normed = widened * lax.rsqrt(lax.optimization_barrier(jnp.mean(widened * widened, axis=-1, keepdims=True)) + norm_eps)
    return (normed * gain_row * (1.0 + scale_row) + shift_row).astype(jnp.bfloat16)

def differential(queries, key_value_rows, share_value, head_gain):
    ratios = []
    for which_map in range(2):
        offset = which_map * HEAD
        scores = jnp.dot(queries[:, offset:offset + HEAD], key_value_rows[:, offset:offset + HEAD].T, preferred_element_type=jnp.float32) * HEAD ** (-0.5)
        powers = jnp.exp(scores)
        weighted = jnp.dot(powers.astype(jnp.bfloat16), key_value_rows[:, VALUE:], preferred_element_type=jnp.float32)
        ratios.append(weighted / lax.optimization_barrier(jnp.sum(powers, axis=1, keepdims=True)))
    difference = ratios[0] - share_value * ratios[1]
    normed = difference * lax.rsqrt(lax.optimization_barrier(jnp.mean(difference * difference, axis=1, keepdims=True)) + head_eps)
    return (normed * head_gain * head_scale).astype(jnp.bfloat16)

def reference(latents, context, condition, context_condition, norm_gain, shift_weight, scale_weight, gate_weight, query_weight, key_weight, value_weight, subtract_share, head_gain, output_weight):
    activated = jax.nn.silu(jnp.stack([condition, context_condition])).astype(jnp.bfloat16)
    shift_terms = jnp.dot(activated, shift_weight, preferred_element_type=jnp.float32)
    scale_terms = jnp.dot(activated, scale_weight, preferred_element_type=jnp.float32)
    gate_terms = jnp.dot(activated, gate_weight, preferred_element_type=jnp.float32)
    latent_mod = modulate(latents, norm_gain, shift_terms[0], scale_terms[0])
    context_mod = modulate(context, norm_gain, shift_terms[1], scale_terms[1])
    cosine, sine_table = rotary_tables(jnp.arange(TOKENS, dtype=jnp.int32))
    block_rows = math.gcd(TOKENS, 512)

    def add_head(head_index, running):
        first_column = jnp.asarray(head_index, jnp.int32) * VALUE

        def columns(weight):
            return lax.dynamic_slice_in_dim(weight, first_column, VALUE, 1)
        latent_query = jnp.dot(latent_mod, columns(query_weight), preferred_element_type=jnp.float32)
        queries = rotate(latent_query.reshape(TOKENS, 2, HEAD), cosine, sine_table)
        queries = queries.reshape(TOKENS, VALUE).astype(jnp.bfloat16)
        latent_key = jnp.dot(latent_mod, columns(key_weight), preferred_element_type=jnp.float32)
        latent_keys = rotate(latent_key.reshape(TOKENS, 2, HEAD), cosine, sine_table)
        latent_keys = latent_keys.reshape(TOKENS, VALUE).astype(jnp.bfloat16)
        latent_values = jnp.dot(latent_mod, columns(value_weight), preferred_element_type=jnp.float32).astype(jnp.bfloat16)
        context_keys = jnp.dot(context_mod, columns(key_weight), preferred_element_type=jnp.float32).astype(jnp.bfloat16)
        context_values = jnp.dot(context_mod, columns(value_weight), preferred_element_type=jnp.float32).astype(jnp.bfloat16)
        key_value_rows = jnp.concatenate([jnp.concatenate([context_keys, context_values], axis=1), jnp.concatenate([latent_keys, latent_values], axis=1)], axis=0)
        share_value = lax.dynamic_index_in_dim(subtract_share, jnp.asarray(head_index, jnp.int32), 0, keepdims=False)

        def one_block(query_block):
            return differential(query_block, key_value_rows, share_value, head_gain)
        head_output = lax.map(one_block, queries.reshape(TOKENS // block_rows, block_rows, VALUE))
        head_output = head_output.reshape(TOKENS, VALUE)
        output_rows = lax.dynamic_slice_in_dim(output_weight, first_column, VALUE, 0)
        return running + jnp.dot(head_output, output_rows, preferred_element_type=jnp.float32)
    branch = lax.fori_loop(0, HEADS, add_head, jnp.zeros((TOKENS, D), jnp.float32))
    return (latents.astype(jnp.float32) + gate_terms[0] * branch).astype(jnp.bfloat16)
```

```python
import functools

import jax
import jax.numpy as jnp
from jax import lax
from jax.experimental import pallas as pl
from jax.experimental.pallas import tpu as pltpu
from jax.sharding import PartitionSpec as P

MESH = pl.DeviceIdType.MESH
HEAD = 64
VALUE = 128
GRID_W = 64

norm_eps = 1e-06
head_eps = 1e-05
rope_theta = 10000.0
head_scale = 0.8
F32 = jnp.float32
BF16 = jnp.bfloat16


def iota(shape, dim):
    return lax.broadcasted_iota(jnp.int32, shape, dim)


def when(condition, action):
    if isinstance(condition, bool):
        if condition:
            action()
    else:
        pl.when(condition)(action)


def remote(src, dst, send_sem, recv_sem, device):
    return pltpu.make_async_remote_copy(
        src_ref=src,
        dst_ref=dst,
        send_sem=send_sem,
        recv_sem=recv_sem,
        device_id=device,
        device_id_type=MESH,
    )


class Exchange:
    def __init__(self, me, count, device_of, source, target, send_sems, recv_sems):
        self.me, self.count, self.device_of = me, count, device_of
        self.source, self.target = source, target
        self.send_sems, self.recv_sems = send_sems, recv_sems

    def copy(self, step):
        peer = lax.rem(self.me + step, self.count)
        return remote(
            self.source(peer),
            self.target(self.me),
            self.send_sems.at[step],
            self.recv_sems.at[self.me],
            self.device_of(peer),
        )

    def steps(self):
        return sorted(range(1, self.count), key=lambda s: -min(s, self.count - s))

    def start(self):
        for step in self.steps():
            self.copy(step).start()

    def wait_recv(self):
        for step in self.steps():
            peer = lax.rem(self.me + step, self.count)
            remote(
                self.target(peer),
                self.target(peer),
                self.send_sems.at[step],
                self.recv_sems.at[peer],
                self.device_of(peer),
            ).wait_recv()

    def wait_send(self):
        for step in self.steps():
            self.copy(step).wait_send()


class Ring:
    def __init__(self, me, count, device_of, view, pieces, right_sems, left_sems, recv_sems):
        self.me, self.count, self.device_of, self.view = me, count, device_of, view
        self.pieces, self.half = pieces, count // 2
        self.right_sems, self.left_sems, self.recv_sems = right_sems, left_sems, recv_sems

    def source(self, step, right):
        return lax.rem(self.me + self.count + (-step if right else step), self.count)

    def carries(self, step, piece, right):
        mine = (piece < self.pieces // 2) == right if self.pieces > 1 else right
        last = self.half if mine else self.half - 1
        return step <= last

    def copy(self, step, piece, right):
        place = self.view(self.source(step, right), piece)
        peer = lax.rem(self.me + (1 if right else self.count - 1), self.count)
        sems = self.right_sems if right else self.left_sems
        return remote(
            place,
            place,
            sems.at[step, piece],
            self.recv_sems.at[self.source(step, right), piece],
            self.device_of(peer),
        )

    def send(self, step, piece, right):
        when(
            self.carries(step + 1, piece, right),
            lambda: self.copy(step, piece, right).start(),
        )

    def send_own(self, piece):
        self.send(0, piece, True)
        self.send(0, piece, False)

    def arrive(self, step, piece, right, then=None):
        def go():
            self.copy(step, piece, right).wait_recv()
            self.send(step, piece, right)
            if then is not None:
                then(step, piece, right)

        when(self.carries(step, piece, right), go)

    def arrive_step(self, step, then=None):
        for piece in range(self.pieces):
            self.arrive(step, piece, True, then)
            self.arrive(step, piece, False, then)

    def wait_send(self):
        for step in range(self.half):
            for piece in range(self.pieces):
                for right in (True, False):
                    if self.carries(step + 1, piece, right):
                        self.copy(step, piece, right).wait_send()


def kernel(
    sizes,
    lat,
    ctx,
    cond,
    ctx_cond,
    gain,
    shift_w,
    scale_w,
    gate_w,
    query_w,
    key_w,
    value_w,
    share,
    head_gain,
    out_w,
    out,
    weights,
    out_weights,
    spread,
    part,
    line_terms,
    all_terms,
    lat_line,
    lat_flat,
    lat_all,
    modded,
    cosines,
    sines_up,
    sines_down,
    order,
    queries,
    pairs,
    sums,
    totals,
    heads_out,
    heads_in,
    rows_out,
    rows_in,
    local_sems,
    part_send,
    part_recv,
    line_send,
    line_recv,
    all_send,
    all_recv,
    lat_send,
    lat_recv,
    z_right,
    z_left,
    z_recv,
    w_right,
    w_left,
    w_across,
    w_recv,
    x_right,
    x_left,
    x_across,
    x_recv,
    heads_send,
    heads_recv,
    rows_send,
    rows_recv,
):
    nx, ny, nz = sizes
    nsp = 2 * nx
    rows, width = lat.shape
    line_rows = ny * rows
    count = nz * line_rows
    ctx_rows = ctx.shape[0]
    sp, tp = lax.axis_index("sp"), lax.axis_index("tp")
    x, core = sp // 2, lax.rem(sp, 2)
    z, y = tp // ny, lax.rem(tp, ny)
    other_sp = x * 2 + 1 - core
    sibling = {"sp": other_sp, "tp": tp}

    def on_sp(peer):
        return {"sp": peer, "tp": tp}

    def on_x(peer):
        return {"sp": peer * 2 + core, "tp": tp}

    def on_y(peer):
        return {"sp": sp, "tp": z * ny + peer}

    def on_z(peer):
        return {"sp": sp, "tp": peer * ny + y}

    barrier = pltpu.get_barrier_semaphore()
    for me, size, device_of in ((sp, nsp, on_sp), (y, ny, on_y), (z, nz, on_z)):
        for step in range(1, size):
            pl.semaphore_signal(
                barrier,
                inc=1,
                device_id=device_of(lax.rem(me + step, size)),
                device_id_type=MESH,
            )

    own_half = out_w.shape[0] // 2
    half_rows = own_half // 2
    local = [
        pltpu.make_async_copy(matrix, weights.at[:, pl.ds(i * VALUE, VALUE)], local_sems.at[i])
        for i, matrix in enumerate((query_w, key_w, value_w))
    ]
    for half in range(2):
        for piece in range(2):
            local.append(
                pltpu.make_async_copy(
                    out_w.at[pl.ds(half * own_half + piece * half_rows, half_rows)],
                    out_weights.at[y, half, piece],
                    local_sems.at[3 + 2 * half + piece],
                )
            )
    for copy in local:
        copy.start()

    columns = shift_w.shape[1]
    group = 128 // columns
    tiles = ny // group
    raw = jnp.where(iota((8, cond.shape[1]), 0) == 0, cond[...], ctx_cond[...])
    activated = (raw / (1.0 + jnp.exp(-raw))).astype(BF16)
    spread[...] = jnp.zeros_like(spread)
    for kind, matrix in enumerate((shift_w, scale_w, gate_w)):
        term = jnp.dot(activated, matrix[...], preferred_element_type=F32)[0:2]
        for place in range(group):
            spread[2 * kind : 2 * kind + 2, place * columns : (place + 1) * columns] = term
    here = iota((8, 128), 1) // columns == lax.rem(y, group)
    part[sp] = jnp.where(here, spread[...], 0.0)
    lat_line[y] = lat[...]

    pl.semaphore_wait(barrier, nsp - 1 + ny - 1 + nz - 1)

    part_exchange = Exchange(
        sp, nsp, on_sp, lambda peer: part.at[sp], lambda me: part.at[me], part_send, part_recv
    )
    lat_exchange = Exchange(
        y, ny, on_y, lambda peer: lat, lambda me: lat_line.at[me], lat_send, lat_recv
    )
    line_exchange = Exchange(
        y,
        ny,
        on_y,
        lambda peer: line_terms.at[y],
        lambda me: line_terms.at[me],
        line_send,
        line_recv,
    )
    all_exchange = Exchange(
        z, nz, on_z, lambda peer: all_terms.at[z], lambda me: all_terms.at[me], all_send, all_recv
    )
    heads_exchange = Exchange(
        y,
        ny,
        on_y,
        lambda peer: heads_out.at[peer],
        lambda me: heads_in.at[me],
        heads_send,
        heads_recv,
    )
    rows_exchange = Exchange(
        z, nz, on_z, lambda peer: rows_out.at[peer], lambda me: rows_in.at[me], rows_send, rows_recv
    )
    half_line = line_rows // 2
    lat_ring = Ring(
        z,
        nz,
        on_z,
        lambda source, piece: lat_all.at[source, pl.ds(piece * half_line, half_line)],
        2,
        z_right,
        z_left,
        z_recv,
    )
    weight_ring = Ring(
        y,
        ny,
        on_y,
        lambda source, piece: out_weights.at[source, core, piece],
        2,
        w_right,
        w_left,
        w_recv.at[0],
    )

    def weight_across(step, piece, right):
        place = out_weights.at[weight_ring.source(step, right), core, piece]
        return remote(
            place,
            place,
            w_across.at[1 if right else 0, step, piece],
            w_recv.at[1, weight_ring.source(step, right), piece],
            sibling,
        )

    def send_weight_across(step, piece, right):
        weight_across(step, piece, right).start()

    near = [0]
    for step in range(1, lat_ring.half // 2 + 1):
        near += [-step, step]
    far = [d for d in range(-(lat_ring.half - 1), lat_ring.half + 1) if d not in near]
    near_rows, far_rows = len(near) * line_rows, len(far) * line_rows
    bounds = (
        (0, ctx_rows),
        (ctx_rows, near_rows // 2),
        (ctx_rows + near_rows // 2, near_rows // 2),
        (ctx_rows + near_rows, far_rows),
    )

    def pair_view(source, piece):
        first, size = bounds[piece]
        return pairs.at[source, pl.ds(first, size)]

    pair_ring = Ring(
        x,
        nx,
        on_x,
        lambda source, piece: pair_view(source * 2 + core, piece),
        4,
        x_right,
        x_left,
        x_recv.at[0],
    )

    def pair_across(step, piece, right):
        source = pair_ring.source(step, right)
        place = pair_view(source * 2 + core, piece)
        return remote(
            place,
            place,
            x_across.at[1 if right else 0, step, piece],
            x_recv.at[1, source, piece],
            sibling,
        )

    def send_pair_across(step, piece, right):
        pair_across(step, piece, right).start()

    def send_pair(piece):
        pair_ring.send_own(piece)
        send_pair_across(0, piece, True)

    part_exchange.start()
    lat_exchange.start()

    token = iota((count, VALUE), 0)
    lane = iota((count, VALUE), 1)
    position = sp * count + token
    quarter = HEAD // 4
    frequency = jnp.exp(
        lax.rem(lane, quarter).astype(F32) * (-2.0 / (HEAD // 2) * jnp.log(F32(rope_theta)))
    )
    place = jnp.where(
        lax.rem(lane, HEAD) < HEAD // 2, position // GRID_W, lax.rem(position, GRID_W)
    )
    angle = place.astype(F32) * frequency
    cosines[...] = jnp.cos(angle).reshape(cosines.shape)
    sine = jnp.sin(angle)
    even = lax.rem(lane // quarter, 2) == 0
    sines_up[...] = jnp.where(even, -sine, 0.0).reshape(sines_up.shape)
    sines_down[...] = jnp.where(even, 0.0, sine).reshape(sines_down.shape)
    to = iota((count, count), 0)
    source = (lax.rem(to // rows, nz) * ny + to // (rows * nz)) * rows + lax.rem(to, rows)
    order[...] = jnp.where(iota((count, count), 1) == source, 1.0, 0.0).astype(BF16)
    sums[...] = jnp.zeros_like(sums)
    totals[...] = jnp.zeros_like(totals)

    part_exchange.wait_recv()
    total = part[0]
    for i in range(1, nsp):
        total = total + part[i]
    line_terms[y] = total
    line_exchange.start()

    lat_exchange.wait_recv()
    for i in range(ny):
        lat_flat[i * rows : (i + 1) * rows, :] = lat_line[i].astype(F32)
    lat_all[z] = lat_flat[...].astype(BF16)
    for piece in range(2):
        lat_ring.send_own(piece)

    for copy in local:
        copy.wait()
    for piece in range(2):
        weight_ring.send_own(piece)

    line_exchange.wait_recv()
    for tile in range(tiles):
        total = line_terms[tile * group]
        for i in range(1, group):
            total = total + line_terms[tile * group + i]
        all_terms[z, tile] = total
    all_exchange.start()

    first_steps = lat_ring.half // 2
    for step in range(1, first_steps + 1):
        lat_ring.arrive_step(step)

    all_exchange.wait_recv()

    def term(row):
        return jnp.concatenate(
            [all_terms[i, tile, row : row + 1, :] for i in range(nz) for tile in range(tiles)], axis=1
        )

    def modulate(token_rows, which):
        widened = token_rows.astype(F32)
        normed = widened * lax.rsqrt(jnp.mean(widened * widened, axis=-1, keepdims=True) + norm_eps)
        return (normed * (gain[...] * (1.0 + term(2 + which))) + term(which)).astype(BF16)

    modded[0:ctx_rows, :] = modulate(ctx[...], 1)
    pairs[sp, 0:ctx_rows, :] = jnp.dot(
        modded[0:ctx_rows, :], weights[:, VALUE:], preferred_element_type=F32
    ).astype(BF16)
    send_pair(0)

    def project(blocks, first):
        size = len(blocks) * line_rows
        places = [lax.rem(z + d + nz, nz) for d in blocks]
        for i, block in enumerate(places):
            modded[i * line_rows : (i + 1) * line_rows, :] = modulate(lat_all[block], 0)
        projected = jnp.dot(modded[0:size, :], weights[...], preferred_element_type=F32)
        for i, block in enumerate(places):
            piece = projected[i * line_rows : (i + 1) * line_rows]
            cosine, up, down = cosines[block], sines_up[block], sines_down[block]

            def rotate(vectors):
                return (
                    vectors * cosine
                    + pltpu.roll(vectors, VALUE - quarter, 1) * up
                    + pltpu.roll(vectors, quarter, 1) * down
                )

            query = rotate(piece[:, :VALUE]).astype(BF16).astype(F32) * HEAD ** (-0.5)
            low = iota(query.shape, 1) < HEAD
            queries[0, block] = jnp.where(low, query, 0.0).astype(BF16)
            queries[1, block] = jnp.where(low, 0.0, query).astype(BF16)
            here = slice(first + i * line_rows, first + (i + 1) * line_rows)
            pairs[sp, here, 0:VALUE] = rotate(piece[:, VALUE : 2 * VALUE]).astype(BF16)
            pairs[sp, here, VALUE:] = piece[:, 2 * VALUE :].astype(BF16)

    project(near, ctx_rows)
    send_pair(1)
    send_pair(2)
    for step in range(first_steps + 1, lat_ring.half + 1):
        lat_ring.arrive_step(step)
    project(far, ctx_rows + near_rows)
    send_pair(3)

    def attend(chip):
        for piece in range(4):
            remote(
                pair_view(chip * 2 + 1 - core, piece),
                pair_view(chip * 2 + 1 - core, piece),
                x_across.at[0, 0, piece],
                x_recv.at[1, chip, piece],
                sibling,
            ).wait_recv()
        block = pairs[pl.ds(chip * 2, 2)]
        block = block.reshape(block.shape[0] * block.shape[1], block.shape[2])
        scores = lax.dot_general(
            queries[...].reshape(2 * count, VALUE),
            block[:, :VALUE],
            (((1,), (1,)), ((), ())),
            preferred_element_type=F32,
        )
        powers = jnp.exp(scores)
        sums[...] += jnp.dot(powers.astype(BF16), block[:, VALUE:], preferred_element_type=F32)
        totals[...] += jnp.sum(powers, axis=1, keepdims=True)

    @pl.loop(1, pair_ring.half + 2)
    def _(step):
        def arrive(piece):
            pair_ring.arrive(step, piece, True, send_pair_across)
            pair_ring.arrive(step, piece, False, send_pair_across)

        arrive(0)
        arrive(1)
        attend(pair_ring.source(step - 1, True))
        arrive(2)
        arrive(3)
        for weight_step in range(1, weight_ring.half):
            when(
                step == min(weight_step, pair_ring.half),
                lambda: weight_ring.arrive_step(weight_step, send_weight_across),
            )
        when(
            (step >= 2) & (step <= pair_ring.half),
            lambda: attend(pair_ring.source(step - 1, False)),
        )

    ratio = sums[...] / totals[...]
    difference = ratio[:count] - share[0] * ratio[count:]
    normed = difference * lax.rsqrt(
        jnp.mean(difference * difference, axis=1, keepdims=True) + head_eps
    )
    head_output = (normed * head_gain[...] * head_scale).astype(BF16)
    heads_out[...] = (
        jnp.dot(order[...], head_output, preferred_element_type=F32)
        .astype(BF16)
        .reshape(heads_out.shape)
    )
    heads_in[y] = heads_out[y]
    heads_exchange.start()

    weight_ring.arrive_step(weight_ring.half, send_weight_across)

    def moves(ring):
        for step in range(1, ring.half + 1):
            for piece in range(ring.pieces):
                for right in (True, False):
                    if ring.carries(step, piece, right):
                        yield step, piece, right

    for step, piece, right in moves(weight_ring):
        source = weight_ring.source(step, right)
        remote(
            out_weights.at[source, 1 - core, piece],
            out_weights.at[source, 1 - core, piece],
            w_across.at[0, 0, piece],
            w_recv.at[1, source, piece],
            sibling,
        ).wait_recv()
    heads_exchange.wait_recv()
    branch = jnp.dot(
        jnp.concatenate([heads_in[i] for i in range(ny)], axis=1),
        out_weights[...].reshape(ny * VALUE, width),
        preferred_element_type=F32,
    )
    for i in range(nz):
        rows_out[i] = branch[i * rows : (i + 1) * rows].astype(BF16)
    rows_in[z] = rows_out[z]
    rows_exchange.start()

    for exchange in (part_exchange, lat_exchange, line_exchange, all_exchange, heads_exchange):
        exchange.wait_send()
    for ring in (lat_ring, weight_ring, pair_ring):
        ring.wait_send()
    for step, piece, right in moves(weight_ring):
        weight_across(step, piece, right).wait_send()
    for piece in range(4):
        pair_across(0, piece, True).wait_send()
    for step, piece, right in moves(pair_ring):
        pair_across(step, piece, right).wait_send()

    rows_exchange.wait_recv()
    total = rows_in[0].astype(F32)
    for i in range(1, nz):
        total = total + rows_in[i].astype(F32)
    out[...] = (lat[...].astype(F32) + term(4) * total).astype(out.dtype)
    rows_exchange.wait_send()


def shards(
    sizes,
    latents,
    context,
    condition,
    context_condition,
    norm_gain,
    shift_weight,
    scale_weight,
    gate_weight,
    query_weight,
    key_weight,
    value_weight,
    subtract_share,
    head_gain,
    output_weight,
):
    nx, ny, nz = sizes
    nsp = 2 * nx
    rows, width = latents.shape
    line_rows = ny * rows
    count = nz * line_rows
    ctx_rows = context.shape[0]
    keys = count + ctx_rows
    tiles = ny * shift_weight.shape[1] // 128
    half = output_weight.shape[0] // 2
    vmem = pl.BlockSpec(memory_space=pltpu.VMEM)
    any_space = pl.BlockSpec(memory_space=pl.ANY)
    smem = pl.BlockSpec(memory_space=pltpu.SMEM)
    dma = pltpu.SemaphoreType.DMA
    hx, hy, hz = max(nx // 2, 1), max(ny // 2, 1), max(nz // 2, 1)
    scratch = [
        pltpu.VMEM((width, 3 * VALUE), BF16),
        pltpu.VMEM((ny, 2, 2, half // 2, width), BF16),
        pltpu.VMEM((8, 128), F32),
        pltpu.VMEM((nsp, 8, 128), F32),
        pltpu.VMEM((ny, 8, 128), F32),
        pltpu.VMEM((nz, tiles, 8, 128), F32),
        pltpu.VMEM((ny, rows, width), BF16),
        pltpu.VMEM((line_rows, width), F32),
        pltpu.VMEM((nz, line_rows, width), BF16),
        pltpu.VMEM((keys, width), BF16),
        pltpu.VMEM((nz, line_rows, VALUE), F32),
        pltpu.VMEM((nz, line_rows, VALUE), F32),
        pltpu.VMEM((nz, line_rows, VALUE), F32),
        pltpu.VMEM((count, count), BF16),
        pltpu.VMEM((2, nz, line_rows, VALUE), BF16),
        pltpu.VMEM((nsp, keys, 2 * VALUE), BF16),
        pltpu.VMEM((2 * count, VALUE), F32),
        pltpu.VMEM((2 * count, 1), F32),
        pltpu.VMEM((ny, nz * rows, VALUE), BF16),
        pltpu.VMEM((ny, nz * rows, VALUE), BF16),
        pltpu.VMEM((nz, rows, width), BF16),
        pltpu.VMEM((nz, rows, width), BF16),
        dma((7,)),
        dma((nsp,)),
        dma((nsp,)),
        dma((ny,)),
        dma((ny,)),
        dma((nz,)),
        dma((nz,)),
        dma((ny,)),
        dma((ny,)),
        dma((hz, 2)),
        dma((hz, 2)),
        dma((nz, 2)),
        dma((hy, 2)),
        dma((hy, 2)),
        dma((2, hy + 1, 2)),
        dma((2, ny, 2)),
        dma((hx, 4)),
        dma((hx, 4)),
        dma((2, hx + 1, 4)),
        dma((2, nx, 4)),
        dma((ny,)),
        dma((ny,)),
        dma((nz,)),
        dma((nz,)),
    ]
    return pl.pallas_call(
        functools.partial(kernel, sizes),
        out_shape=jax.ShapeDtypeStruct(latents.shape, latents.dtype),
        in_specs=[vmem] * 8 + [any_space] * 3 + [smem, vmem, any_space],
        out_specs=vmem,
        scratch_shapes=scratch,
        compiler_params=pltpu.CompilerParams(
            collective_id=0, has_side_effects=True, vmem_limit_bytes=48 * 2**20
        ),
    )(
        latents,
        context,
        condition.reshape(1, -1),
        context_condition.reshape(1, -1),
        norm_gain.reshape(1, -1),
        shift_weight,
        scale_weight,
        gate_weight,
        query_weight,
        key_weight,
        value_weight,
        subtract_share,
        head_gain.reshape(1, -1),
        output_weight,
    )


def solution(mesh):
    nsp, ntp = mesh.shape["sp"], mesh.shape["tp"]
    side = int(round(ntp**0.5))
    sizes = (nsp // 2, side, ntp // side)
    in_specs = (
        P(("sp", "tp"), None),
        P("sp", None),
        P("sp"),
        P("sp"),
        P(),
        P("sp", "tp"),
        P("sp", "tp"),
        P("sp", "tp"),
        P(None, "tp"),
        P(None, "tp"),
        P(None, "tp"),
        P("tp"),
        P(),
        P("tp", None),
    )
    out_specs = P(("sp", "tp"), None)
    return jax.shard_map(
        functools.partial(shards, sizes),
        mesh=mesh,
        in_specs=in_specs,
        out_specs=out_specs,
        check_vma=False,
    )
```

```python
import functools

import jax
import jax.numpy as jnp
from jax import lax
from jax.experimental import pallas as pl
from jax.experimental.pallas import tpu as pltpu
from jax.sharding import PartitionSpec as P

MESH = pl.DeviceIdType.MESH
HEAD = 64
VALUE = 128
GRID_W = 64

norm_eps = 1e-06
head_eps = 1e-05
rope_theta = 10000.0
head_scale = 0.8
F32 = jnp.float32
BF16 = jnp.bfloat16


def iota(shape, dim):
    return lax.broadcasted_iota(jnp.int32, shape, dim)


def when(condition, action):
    if isinstance(condition, bool):
        if condition:
            action()
    else:
        pl.when(condition)(action)


def remote(src, dst, send_sem, recv_sem, device):
    return pltpu.make_async_remote_copy(
        src_ref=src,
        dst_ref=dst,
        send_sem=send_sem,
        recv_sem=recv_sem,
        device_id=device,
        device_id_type=MESH,
    )


class Exchange:
    def __init__(self, me, count, device_of, source, target, send_sems, recv_sems):
        self.me, self.count, self.device_of = me, count, device_of
        self.source, self.target = source, target
        self.send_sems, self.recv_sems = send_sems, recv_sems

    def copy(self, step):
        peer = lax.rem(self.me + step, self.count)
        return remote(
            self.source(peer),
            self.target(self.me),
            self.send_sems.at[step],
            self.recv_sems.at[self.me],
            self.device_of(peer),
        )

    def steps(self):
        return sorted(range(1, self.count), key=lambda s: -min(s, self.count - s))

    def start(self):
        for step in self.steps():
            self.copy(step).start()

    def wait_recv(self):
        for step in self.steps():
            peer = lax.rem(self.me + step, self.count)
            remote(
                self.target(peer),
                self.target(peer),
                self.send_sems.at[step],
                self.recv_sems.at[peer],
                self.device_of(peer),
            ).wait_recv()

    def wait_send(self):
        for step in self.steps():
            self.copy(step).wait_send()


class Ring:
    def __init__(self, me, count, device_of, view, pieces, right_sems, left_sems, recv_sems):
        self.me, self.count, self.device_of, self.view = me, count, device_of, view
        self.pieces, self.half = pieces, count // 2
        self.right_sems, self.left_sems, self.recv_sems = right_sems, left_sems, recv_sems

    def source(self, step, right):
        return lax.rem(self.me + self.count + (-step if right else step), self.count)

    def carries(self, step, piece, right):
        mine = (piece < self.pieces // 2) == right if self.pieces > 1 else right
        last = self.half if mine else self.half - 1
        return step <= last

    def copy(self, step, piece, right):
        place = self.view(self.source(step, right), piece)
        peer = lax.rem(self.me + (1 if right else self.count - 1), self.count)
        sems = self.right_sems if right else self.left_sems
        return remote(
            place,
            place,
            sems.at[step, piece],
            self.recv_sems.at[self.source(step, right), piece],
            self.device_of(peer),
        )

    def send(self, step, piece, right):
        when(
            self.carries(step + 1, piece, right),
            lambda: self.copy(step, piece, right).start(),
        )

    def send_own(self, piece):
        self.send(0, piece, True)
        self.send(0, piece, False)

    def arrive(self, step, piece, right, then=None):
        def go():
            self.copy(step, piece, right).wait_recv()
            self.send(step, piece, right)
            if then is not None:
                then(step, piece, right)

        when(self.carries(step, piece, right), go)

    def arrive_step(self, step, then=None):
        for piece in range(self.pieces):
            self.arrive(step, piece, True, then)
            self.arrive(step, piece, False, then)

    def wait_send(self):
        for step in range(self.half):
            for piece in range(self.pieces):
                for right in (True, False):
                    if self.carries(step + 1, piece, right):
                        self.copy(step, piece, right).wait_send()


def kernel(
    sizes,
    lat_hbm,
    ctx_hbm,
    cond_hbm,
    ctx_cond_hbm,
    gain_hbm,
    shift_hbm,
    scale_hbm,
    gate_hbm,
    query_w,
    key_w,
    value_w,
    share_hbm,
    head_gain_hbm,
    out_w,
    out,
    ctx,
    cond,
    ctx_cond,
    gain,
    shift_w,
    scale_w,
    gate_w,
    head_gain,
    share,
    weights,
    out_weights,
    spread,
    part,
    line_terms,
    all_terms,
    lat_line,
    lat_flat,
    lat_all,
    modded,
    cosines,
    sines_up,
    sines_down,
    order,
    queries,
    pairs,
    sums,
    totals,
    heads_out,
    heads_in,
    rows_out,
    rows_in,
    local_sems,
    early_sems,
    part_send,
    part_recv,
    line_send,
    line_recv,
    all_send,
    all_recv,
    lat_send,
    lat_recv,
    z_right,
    z_left,
    z_recv,
    w_right,
    w_left,
    w_across,
    w_recv,
    x_right,
    x_left,
    x_across,
    x_recv,
    heads_send,
    heads_recv,
    rows_send,
    rows_recv,
):
    nx, ny, nz = sizes
    nsp = 2 * nx
    rows, width = lat_hbm.shape
    line_rows = ny * rows
    count = nz * line_rows
    ctx_rows = ctx.shape[0]
    sp, tp = lax.axis_index("sp"), lax.axis_index("tp")
    x, core = sp // 2, lax.rem(sp, 2)
    z, y = tp // ny, lax.rem(tp, ny)
    other_sp = x * 2 + 1 - core
    sibling = {"sp": other_sp, "tp": tp}

    def on_sp(peer):
        return {"sp": peer, "tp": tp}

    def on_x(peer):
        return {"sp": peer * 2 + core, "tp": tp}

    def on_y(peer):
        return {"sp": sp, "tp": z * ny + peer}

    def on_z(peer):
        return {"sp": sp, "tp": peer * ny + y}

    early = [
        pltpu.make_async_copy(source, place, early_sems.at[i])
        for i, (source, place) in enumerate(
            (
                (cond_hbm, cond),
                (ctx_cond_hbm, ctx_cond),
                (shift_hbm, shift_w),
                (scale_hbm, scale_w),
                (gate_hbm, gate_w),
                (lat_hbm, lat_line.at[y]),
            )
        )
    ]
    for copy in early:
        copy.start()

    barrier = pltpu.get_barrier_semaphore()
    for me, size, device_of in ((sp, nsp, on_sp), (y, ny, on_y), (z, nz, on_z)):
        for step in range(1, size):
            pl.semaphore_signal(
                barrier,
                inc=1,
                device_id=device_of(lax.rem(me + step, size)),
                device_id_type=MESH,
            )

    own_half = out_w.shape[0] // 2
    half_rows = own_half // 2
    local = [
        pltpu.make_async_copy(matrix, weights.at[:, pl.ds(i * VALUE, VALUE)], local_sems.at[i])
        for i, matrix in enumerate((query_w, key_w, value_w))
    ]
    for half in range(2):
        for piece in range(2):
            local.append(
                pltpu.make_async_copy(
                    out_w.at[pl.ds(half * own_half + piece * half_rows, half_rows)],
                    out_weights.at[y, half, piece],
                    local_sems.at[3 + 2 * half + piece],
                )
            )
    local.append(pltpu.make_async_copy(ctx_hbm, ctx, local_sems.at[7]))
    local.append(pltpu.make_async_copy(gain_hbm, gain, local_sems.at[8]))
    local.append(pltpu.make_async_copy(head_gain_hbm, head_gain, local_sems.at[9]))
    local.append(pltpu.make_async_copy(share_hbm, share, local_sems.at[10]))
    for copy in local:
        copy.start()
    for copy in early:
        copy.wait()

    columns = shift_w.shape[0]
    group = 128 // columns
    tiles = ny // group
    raw = jnp.where(iota((8, cond.shape[1]), 0) == 0, cond[...], ctx_cond[...])
    activated = (raw / (1.0 + jnp.exp(-raw))).astype(BF16)
    spread[...] = jnp.zeros_like(spread)
    for kind, matrix in enumerate((shift_w, scale_w, gate_w)):
        term = lax.dot_general(
            activated,
            matrix[...],
            (((1,), (1,)), ((), ())),
            preferred_element_type=F32,
        )[0:2]
        for place in range(group):
            spread[2 * kind : 2 * kind + 2, place * columns : (place + 1) * columns] = term
    here = iota((8, 128), 1) // columns == lax.rem(y, group)
    part[sp] = jnp.where(here, spread[...], 0.0)

    pl.semaphore_wait(barrier, nsp - 1 + ny - 1 + nz - 1)

    part_exchange = Exchange(
        sp, nsp, on_sp, lambda peer: part.at[sp], lambda me: part.at[me], part_send, part_recv
    )
    lat_exchange = Exchange(
        y, ny, on_y, lambda peer: lat_line.at[y], lambda me: lat_line.at[me], lat_send, lat_recv
    )
    line_exchange = Exchange(
        y,
        ny,
        on_y,
        lambda peer: line_terms.at[y],
        lambda me: line_terms.at[me],
        line_send,
        line_recv,
    )
    all_exchange = Exchange(
        z, nz, on_z, lambda peer: all_terms.at[z], lambda me: all_terms.at[me], all_send, all_recv
    )
    heads_exchange = Exchange(
        y,
        ny,
        on_y,
        lambda peer: heads_out.at[peer],
        lambda me: heads_in.at[me],
        heads_send,
        heads_recv,
    )
    rows_exchange = Exchange(
        z, nz, on_z, lambda peer: rows_out.at[peer], lambda me: rows_in.at[me], rows_send, rows_recv
    )
    part_line = line_rows // 4
    lat_ring = Ring(
        z,
        nz,
        on_z,
        lambda source, piece: lat_all.at[source, pl.ds(piece * part_line, part_line)],
        4,
        z_right,
        z_left,
        z_recv,
    )
    weight_ring = Ring(
        y,
        ny,
        on_y,
        lambda source, piece: out_weights.at[source, core, piece],
        2,
        w_right,
        w_left,
        w_recv.at[0],
    )

    def weight_across(step, piece, right):
        place = out_weights.at[weight_ring.source(step, right), core, piece]
        return remote(
            place,
            place,
            w_across.at[1 if right else 0, step, piece],
            w_recv.at[1, weight_ring.source(step, right), piece],
            sibling,
        )

    def send_weight_across(step, piece, right):
        weight_across(step, piece, right).start()

    weight_moves = [(step, piece) for step in range(1, weight_ring.half + 1) for piece in range(2)]

    def pass_weights(index):
        if index < len(weight_moves):
            step, piece = weight_moves[index]
            weight_ring.arrive(step, piece, True, send_weight_across)
            weight_ring.arrive(step, piece, False, send_weight_across)

    near = [0]
    for step in range(1, lat_ring.half // 2 + 1):
        near += [-step, step]
    far = [d for d in range(-(lat_ring.half - 1), lat_ring.half + 1) if d not in near]
    near_rows, far_rows = len(near) * line_rows, len(far) * line_rows
    bounds = (
        (0, ctx_rows),
        (ctx_rows, near_rows // 2),
        (ctx_rows + near_rows // 2, near_rows // 2),
        (ctx_rows + near_rows, far_rows),
    )

    def pair_view(source, piece):
        first, size = bounds[piece]
        return pairs.at[source, pl.ds(first, size)]

    pair_ring = Ring(
        x,
        nx,
        on_x,
        lambda source, piece: pair_view(source * 2 + core, piece),
        4,
        x_right,
        x_left,
        x_recv.at[0],
    )

    def pair_across(step, piece, right):
        source = pair_ring.source(step, right)
        place = pair_view(source * 2 + core, piece)
        return remote(
            place,
            place,
            x_across.at[1 if right else 0, step, piece],
            x_recv.at[1, source, piece],
            sibling,
        )

    def send_pair_across(step, piece, right):
        pair_across(step, piece, right).start()

    def send_pair(piece):
        pair_ring.send_own(piece)
        send_pair_across(0, piece, True)

    part_exchange.start()
    lat_exchange.start()

    token = iota((count, VALUE), 0)
    lane = iota((count, VALUE), 1)
    position = sp * count + token
    quarter = HEAD // 4
    frequency = jnp.exp(
        lax.rem(lane, quarter).astype(F32) * (-2.0 / (HEAD // 2) * jnp.log(F32(rope_theta)))
    )
    place = jnp.where(
        lax.rem(lane, HEAD) < HEAD // 2, position // GRID_W, lax.rem(position, GRID_W)
    )
    angle = place.astype(F32) * frequency
    cosines[...] = jnp.cos(angle).reshape(cosines.shape)
    sine = jnp.sin(angle)
    even = lax.rem(lane // quarter, 2) == 0
    sines_up[...] = jnp.where(even, -sine, 0.0).reshape(sines_up.shape)
    sines_down[...] = jnp.where(even, 0.0, sine).reshape(sines_down.shape)
    to = iota((count, count), 0)
    source = (lax.rem(to // rows, nz) * ny + to // (rows * nz)) * rows + lax.rem(to, rows)
    order[...] = jnp.where(iota((count, count), 1) == source, 1.0, 0.0).astype(BF16)
    sums[...] = jnp.zeros_like(sums)
    totals[...] = jnp.zeros_like(totals)

    part_exchange.wait_recv()
    total = part[0]
    for i in range(1, nsp):
        total = total + part[i]
    line_terms[y] = total
    line_exchange.start()

    lat_exchange.wait_recv()
    for i in range(ny):
        lat_flat[i * rows : (i + 1) * rows, :] = lat_line[i].astype(F32)
    lat_all[z] = lat_flat[...].astype(BF16)
    for piece in range(4):
        lat_ring.send_own(piece)

    for copy in local:
        copy.wait()
    for piece in range(2):
        weight_ring.send_own(piece)

    line_exchange.wait_recv()
    for tile in range(tiles):
        total = line_terms[tile * group]
        for i in range(1, group):
            total = total + line_terms[tile * group + i]
        all_terms[z, tile] = total
    all_exchange.start()

    first_steps = lat_ring.half // 2
    for step in range(1, first_steps + 1):
        lat_ring.arrive_step(step)

    all_exchange.wait_recv()
    pass_weights(0)

    def term(row):
        return jnp.concatenate(
            [all_terms[i, tile, row : row + 1, :] for i in range(nz) for tile in range(tiles)], axis=1
        )

    def modulate(token_rows, which):
        widened = token_rows.astype(F32)
        normed = widened * lax.rsqrt(jnp.mean(widened * widened, axis=-1, keepdims=True) + norm_eps)
        return (normed * (gain[...] * (1.0 + term(2 + which))) + term(which)).astype(BF16)

    modded[0:ctx_rows, :] = modulate(ctx[...], 1)
    pairs[sp, 0:ctx_rows, :] = jnp.dot(
        modded[0:ctx_rows, :], weights[:, VALUE:], preferred_element_type=F32
    ).astype(BF16)
    send_pair(0)

    def project(blocks, first):
        size = len(blocks) * line_rows
        places = [lax.rem(z + d + nz, nz) for d in blocks]
        for i, block in enumerate(places):
            modded[i * line_rows : (i + 1) * line_rows, :] = modulate(lat_all[block], 0)
        projected = jnp.dot(modded[0:size, :], weights[...], preferred_element_type=F32)
        for i, block in enumerate(places):
            piece = projected[i * line_rows : (i + 1) * line_rows]
            cosine, up, down = cosines[block], sines_up[block], sines_down[block]

            def rotate(vectors):
                return (
                    vectors * cosine
                    + pltpu.roll(vectors, VALUE - quarter, 1) * up
                    + pltpu.roll(vectors, quarter, 1) * down
                )

            query = rotate(piece[:, :VALUE]).astype(BF16).astype(F32) * HEAD ** (-0.5)
            low = iota(query.shape, 1) < HEAD
            queries[0, block] = jnp.where(low, query, 0.0).astype(BF16)
            queries[1, block] = jnp.where(low, 0.0, query).astype(BF16)
            here = slice(first + i * line_rows, first + (i + 1) * line_rows)
            pairs[sp, here, 0:VALUE] = rotate(piece[:, VALUE : 2 * VALUE]).astype(BF16)
            pairs[sp, here, VALUE:] = piece[:, 2 * VALUE :].astype(BF16)

    project(near, ctx_rows)
    send_pair(1)
    send_pair(2)
    pass_weights(1)
    for step in range(first_steps + 1, lat_ring.half + 1):
        lat_ring.arrive_step(step)
    project(far, ctx_rows + near_rows)
    send_pair(3)
    pass_weights(2)

    def attend(chip):
        for piece in range(4):
            remote(
                pair_view(chip * 2 + 1 - core, piece),
                pair_view(chip * 2 + 1 - core, piece),
                x_across.at[0, 0, piece],
                x_recv.at[1, chip, piece],
                sibling,
            ).wait_recv()
        block = pairs[pl.ds(chip * 2, 2)]
        block = block.reshape(block.shape[0] * block.shape[1], block.shape[2])
        scores = lax.dot_general(
            queries[...].reshape(2 * count, VALUE),
            block[:, :VALUE],
            (((1,), (1,)), ((), ())),
            preferred_element_type=F32,
        )
        powers = jnp.exp(scores)
        sums[...] += jnp.dot(powers.astype(BF16), block[:, VALUE:], preferred_element_type=F32)
        totals[...] += jnp.sum(powers, axis=1, keepdims=True)

    @pl.loop(1, pair_ring.half + 2)
    def _(step):
        def arrive(piece):
            pair_ring.arrive(step, piece, True, send_pair_across)
            pair_ring.arrive(step, piece, False, send_pair_across)

        arrive(0)
        arrive(1)
        pl.when(step >= 2)(lambda: attend(pair_ring.source(step - 1, True)))
        arrive(2)
        arrive(3)
        for index in (3, 4, 5):
            pl.when(step == min(index - 2, pair_ring.half))(lambda: pass_weights(index))
        pl.when(step <= pair_ring.half)(lambda: attend(pair_ring.source(step - 1, False)))

    ratio = sums[...] / totals[...]
    difference = ratio[:count] - share[...] * ratio[count:]
    normed = difference * lax.rsqrt(
        jnp.mean(difference * difference, axis=1, keepdims=True) + head_eps
    )
    head_output = (normed * head_gain[...] * head_scale).astype(BF16)
    heads_out[...] = (
        jnp.dot(order[...], head_output, preferred_element_type=F32)
        .astype(BF16)
        .reshape(heads_out.shape)
    )
    heads_in[y] = heads_out[y]
    heads_exchange.start()

    pass_weights(6)
    pass_weights(7)

    def moves(ring):
        for step in range(1, ring.half + 1):
            for piece in range(ring.pieces):
                for right in (True, False):
                    if ring.carries(step, piece, right):
                        yield step, piece, right

    for step, piece, right in moves(weight_ring):
        source = weight_ring.source(step, right)
        remote(
            out_weights.at[source, 1 - core, piece],
            out_weights.at[source, 1 - core, piece],
            w_across.at[0, 0, piece],
            w_recv.at[1, source, piece],
            sibling,
        ).wait_recv()
    heads_exchange.wait_recv()
    branch = jnp.dot(
        jnp.concatenate([heads_in[i] for i in range(ny)], axis=1),
        out_weights[...].reshape(ny * VALUE, width),
        preferred_element_type=F32,
    )
    for i in range(nz):
        rows_out[i] = branch[i * rows : (i + 1) * rows].astype(BF16)
    rows_in[z] = rows_out[z]
    rows_exchange.start()

    for exchange in (part_exchange, lat_exchange, line_exchange, all_exchange, heads_exchange):
        exchange.wait_send()
    for ring in (lat_ring, weight_ring, pair_ring):
        ring.wait_send()
    for step, piece, right in moves(weight_ring):
        weight_across(step, piece, right).wait_send()
    for piece in range(4):
        pair_across(0, piece, True).wait_send()
    for step, piece, right in moves(pair_ring):
        pair_across(step, piece, right).wait_send()

    rows_exchange.wait_recv()
    total = rows_in[0].astype(F32)
    for i in range(1, nz):
        total = total + rows_in[i].astype(F32)
    out[...] = (lat_line[y].astype(F32) + term(4) * total).astype(out.dtype)
    rows_exchange.wait_send()


def shards(
    sizes,
    latents,
    context,
    condition,
    context_condition,
    norm_gain,
    shift_weight,
    scale_weight,
    gate_weight,
    query_weight,
    key_weight,
    value_weight,
    subtract_share,
    head_gain,
    output_weight,
):
    nx, ny, nz = sizes
    nsp = 2 * nx
    rows, width = latents.shape
    line_rows = ny * rows
    count = nz * line_rows
    ctx_rows = context.shape[0]
    keys = count + ctx_rows
    tiles = ny * shift_weight.shape[1] // 128
    half = output_weight.shape[0] // 2
    vmem = pl.BlockSpec(memory_space=pltpu.VMEM)
    any_space = pl.BlockSpec(memory_space=pl.ANY)
    dma = pltpu.SemaphoreType.DMA
    hx, hy, hz = max(nx // 2, 1), max(ny // 2, 1), max(nz // 2, 1)
    scratch = [
        pltpu.VMEM(context.shape, BF16),
        pltpu.VMEM((1, condition.size), F32),
        pltpu.VMEM((1, condition.size), F32),
        pltpu.VMEM((1, width), F32),
        pltpu.VMEM(shift_weight.shape[::-1], BF16),
        pltpu.VMEM(shift_weight.shape[::-1], BF16),
        pltpu.VMEM(shift_weight.shape[::-1], BF16),
        pltpu.VMEM((1, VALUE), F32),
        pltpu.VMEM((1, 1), F32),
        pltpu.VMEM((width, 3 * VALUE), BF16),
        pltpu.VMEM((ny, 2, 2, half // 2, width), BF16),
        pltpu.VMEM((8, 128), F32),
        pltpu.VMEM((nsp, 8, 128), F32),
        pltpu.VMEM((ny, 8, 128), F32),
        pltpu.VMEM((nz, tiles, 8, 128), F32),
        pltpu.VMEM((ny, rows, width), BF16),
        pltpu.VMEM((line_rows, width), F32),
        pltpu.VMEM((nz, line_rows, width), BF16),
        pltpu.VMEM((keys, width), BF16),
        pltpu.VMEM((nz, line_rows, VALUE), F32),
        pltpu.VMEM((nz, line_rows, VALUE), F32),
        pltpu.VMEM((nz, line_rows, VALUE), F32),
        pltpu.VMEM((count, count), BF16),
        pltpu.VMEM((2, nz, line_rows, VALUE), BF16),
        pltpu.VMEM((nsp, keys, 2 * VALUE), BF16),
        pltpu.VMEM((2 * count, VALUE), F32),
        pltpu.VMEM((2 * count, 1), F32),
        pltpu.VMEM((ny, nz * rows, VALUE), BF16),
        pltpu.VMEM((ny, nz * rows, VALUE), BF16),
        pltpu.VMEM((nz, rows, width), BF16),
        pltpu.VMEM((nz, rows, width), BF16),
        dma((11,)),
        dma((6,)),
        dma((nsp,)),
        dma((nsp,)),
        dma((ny,)),
        dma((ny,)),
        dma((nz,)),
        dma((nz,)),
        dma((ny,)),
        dma((ny,)),
        dma((hz, 4)),
        dma((hz, 4)),
        dma((nz, 4)),
        dma((hy, 2)),
        dma((hy, 2)),
        dma((2, hy + 1, 2)),
        dma((2, ny, 2)),
        dma((hx, 4)),
        dma((hx, 4)),
        dma((2, hx + 1, 4)),
        dma((2, nx, 4)),
        dma((ny,)),
        dma((ny,)),
        dma((nz,)),
        dma((nz,)),
    ]
    return pl.pallas_call(
        functools.partial(kernel, sizes),
        out_shape=jax.ShapeDtypeStruct(latents.shape, latents.dtype),
        in_specs=[any_space] * 14,
        out_specs=vmem,
        scratch_shapes=scratch,
        compiler_params=pltpu.CompilerParams(
            collective_id=0, has_side_effects=True, vmem_limit_bytes=67043328
        ),
    )(
        latents,
        context,
        condition.reshape(1, -1),
        context_condition.reshape(1, -1),
        norm_gain.reshape(1, -1),
        shift_weight.T,
        scale_weight.T,
        gate_weight.T,
        query_weight,
        key_weight,
        value_weight,
        subtract_share.reshape(1, 1),
        head_gain.reshape(1, -1),
        output_weight,
    )


def solution(mesh):
    nsp, ntp = mesh.shape["sp"], mesh.shape["tp"]
    side = int(round(ntp**0.5))
    sizes = (nsp // 2, side, ntp // side)
    in_specs = (
        P(("sp", "tp"), None),
        P("sp", None),
        P("sp"),
        P("sp"),
        P(),
        P("sp", "tp"),
        P("sp", "tp"),
        P("sp", "tp"),
        P(None, "tp"),
        P(None, "tp"),
        P(None, "tp"),
        P("tp"),
        P(),
        P("tp", None),
    )
    out_specs = P(("sp", "tp"), None)
    return jax.shard_map(
        functools.partial(shards, sizes),
        mesh=mesh,
        in_specs=in_specs,
        out_specs=out_specs,
        check_vma=False,
    )
```
